32 devices in a mesh: sp: 32 (over z, y, x, core), tp: 1.
Axes of the slice: x: 2, y: 2, z: 4, core: 2. Of those that a mesh axis runs over, the one named last changes fastest.
Arguments:
- queries: bfloat16 [4096, 2048], P('sp', 'tp'), may hold values from -6 to 6
- forget_logits: bfloat16 [2, 4096, 2048], P(None, 'sp', 'tp'), may hold values from -7.5 to 7.5
- value_matrix: bfloat16 [4096, 2048], P('sp', 'tp'), may hold values from -6 to 6
- output_gate_logits: bfloat16 [4096, 2048], P('sp', 'tp'), may hold values from -6 to 6
- forget_slack: float32 [2048], P('tp'), may hold values from 0.00012207031 to 0.07
- spike_log_forget: float32 [4096, 16], P('sp', 'tp'), may hold values from -2.8 to 0, as said below
- head_norm_gain: bfloat16 [128], replicated, may hold values from 0.099609375 to 1.8984375
- output_weight: bfloat16 [2048, 2048], P('tp'), may hold values from -0.125 to 0.125
- residual: bfloat16 [4096, 2048], P('sp'), may hold values from -6 to 6
- mixer_norm_gain: bfloat16 [2048], replicated, may hold values from 0.099609375 to 1.8984375
- mixer_gate_weight: bfloat16 [2048, 5632], P('sp', 'tp'), may hold values from -0.125 to 0.125
- mixer_up_weight: bfloat16 [2048, 5632], P('sp', 'tp'), may hold values from -0.125 to 0.125
- mixer_down_weight: bfloat16 [5632, 2048], P('tp', 'sp'), may hold values from -0.078125 to 0.078125
Outputs:
- layer_out: bfloat16 [4096, 2048], P(('sp', 'tp'))
The draws below stay inside these ranges and needn't reach their ends.
Inputs may be any that keep to these rules, and one draw needn't show every extreme that they name: `spike_log_forget`: zero at all but a few tokens.
All inputs are finite; a program needn't handle non-finite values.
Results may differ from the reference program's by a relative error of at most 0.015.
Values may be sent and summed in bfloat16 or wider, within the bound.
A program may use at most 192 MiB of HBM per device.

```python
import jax
import jax.numpy as jnp
from jax import lax

D = 2048
FF = 5632
HEADS = 16
HEAD = 128
BLOCK = 128
TOK_DEV = 128
TOKENS = 4096
N_TP = 1


def quick_heads(key, quick_count):
    pick_key = jax.random.fold_in(jax.random.fold_in(key, 23), 0)
    ordering = jax.random.permutation(pick_key, HEADS)
    return ordering < quick_count


def draw_forget_logits(key, part):
    noise_key, steady_key, slow_key, channel_key = jax.random.split(jax.random.fold_in(key, 11), 4)
    channels = HEADS * HEAD
    blocks_count = TOKENS // TOK_DEV
    quick_count = HEADS // 2
    slow_share = 0.5
    quick = quick_heads(key, quick_count)
    slow_block = jax.random.uniform(slow_key, (2, blocks_count, HEADS), jnp.float32) < slow_share
    quick_shift = jnp.where(slow_block, 6.0, -3.0)
    steady_shift = jax.random.uniform(steady_key, (2, blocks_count, HEADS), jnp.float32, -6.0, 1.5)
    head_shift = jnp.where(quick[None, None, :], quick_shift, steady_shift)
    channel_shift = jax.random.uniform(channel_key, (2, blocks_count, HEADS, HEAD), jnp.float32, -1.0, 1.0)
    shifted = (head_shift[:, :, :, None] + channel_shift).reshape(2, blocks_count, 1, channels)
    noise = jnp.clip(jax.random.normal(noise_key, (2, blocks_count, TOK_DEV, channels), jnp.float32), -6.0, 6.0)
    total = jnp.clip(shifted + noise, -7.5, 7.5)
    return total.reshape(2, TOKENS, channels).astype(jnp.bfloat16)


def draw_forget_slack(key, part):
    fast_key = jax.random.fold_in(jax.random.fold_in(key, 23), 1)
    slow_key = jax.random.fold_in(jax.random.fold_in(key, 23), 2)
    quick_count = HEADS // 2
    quick = quick_heads(key, quick_count)[:, None]
    quick_rate = jnp.exp(jax.random.uniform(fast_key, (HEADS, HEAD), jnp.float32, jnp.log(0.02), jnp.log(0.07)))
    steady_rate = jnp.exp(jax.random.uniform(slow_key, (HEADS, HEAD), jnp.float32, jnp.log(0.5), jnp.log(2.0))) / TOKENS
    return jnp.where(quick, quick_rate, steady_rate).reshape(HEADS * HEAD)


def draw_spike_log_forget(key, part):
    place_key, depth_key = jax.random.split(jax.random.fold_in(key, 37))
    spots = jax.random.randint(place_key, (4,), 0, TOKENS)
    upper = jnp.log(0.8)
    depths = jax.random.uniform(depth_key, (4, HEADS), jnp.float32, jnp.log(0.5), upper)
    hits = (jnp.arange(TOKENS)[:, None] == spots[None, :]).astype(jnp.float32)
    return jnp.dot(hits, depths)


def block_levels(stream_key, dims, pieces, least, top_value):
    def one(axis_at, parts):
        heights = jax.random.uniform(jax.random.fold_in(jax.random.fold_in(stream_key, 6), axis_at), (parts,), jnp.float32, least / len(pieces), top_value / len(pieces))
        return jnp.repeat(jnp.exp(heights), dims[axis_at] // parts).reshape((-1,) + (1,) * (len(dims) - axis_at - 1))

    gain = one(*pieces[0])
    for cut in pieces[1:]:
        gain = gain * one(*cut)
    return gain


def scatter_about(own_key, dims, spread, most, pieces=(), held_as=jnp.bfloat16):
    values = spread * jax.random.normal(own_key, dims, jnp.float32)
    if pieces:
        values = values * block_levels(own_key, dims, pieces, -0.22, 0.18)
    return jnp.clip(values, -most, most).astype(held_as)


def setup_inputs(seed: int = 0) -> dict:
    seeds = jax.random.split(jax.random.key(seed), 14)
    queries = scatter_about(seeds[0], (TOKENS, HEADS * HEAD), 1.0, 6.0, ((0, 32),))
    forget_logits = draw_forget_logits(jax.random.fold_in(seeds[13], 71), 0)
    value_matrix = scatter_about(seeds[2], (TOKENS, HEADS * HEAD), 1.0, 6.0, ((0, 32),))
    output_gate_logits = scatter_about(seeds[3], (TOKENS, HEADS * HEAD), 1.0, 6.0, ((0, 32),))
    forget_slack = draw_forget_slack(jax.random.fold_in(seeds[13], 71), 0)
    spike_log_forget = draw_spike_log_forget(jax.random.fold_in(seeds[13], 71), 0)
    head_norm_gain = jnp.clip(1.0 + 0.18 * jax.random.normal(seeds[6], (HEAD,), jnp.float32), 0.099609375, 1.8984375).astype(jnp.bfloat16)
    output_weight = scatter_about(seeds[7], (HEADS * HEAD, D), (HEADS * HEAD) ** -0.5, 0.125)
    residual = scatter_about(seeds[8], (TOKENS, D), 1.0, 6.0, ((0, 32),))
    mixer_norm_gain = jnp.clip(1.0 + 0.18 * jax.random.normal(seeds[9], (D,), jnp.float32), 0.099609375, 1.8984375).astype(jnp.bfloat16)
    mixer_gate_weight = scatter_about(seeds[10], (D, FF), D ** -0.5, 0.125, ((0, 32),))
    mixer_up_weight = scatter_about(seeds[11], (D, FF), D ** -0.5, 0.125, ((0, 32),))
    mixer_down_weight = scatter_about(seeds[12], (FF, D), FF ** -0.5, 0.078125, ((1, 32),))
    return dict(queries=queries, forget_logits=forget_logits, value_matrix=value_matrix, output_gate_logits=output_gate_logits, forget_slack=forget_slack, spike_log_forget=spike_log_forget, head_norm_gain=head_norm_gain, output_weight=output_weight, residual=residual, mixer_norm_gain=mixer_norm_gain, mixer_gate_weight=mixer_gate_weight, mixer_up_weight=mixer_up_weight, mixer_down_weight=mixer_down_weight)


NORM_EPS = 1e-06
BEST_PRECISION = lax.Precision.HIGHEST

def rms_scale(entries, gain_vec):
    return entries * lax.rsqrt(lax.optimization_barrier(jnp.mean(entries * entries, axis=-1, keepdims=True)) + NORM_EPS) * gain_vec.astype(jnp.float32)

def full_sweep(query_f, key_f, decay_f, value_f):
    total_rows, heads_all, head_width = query_f.shape
    blocks_count = total_rows // BLOCK
    tri_mask = jnp.tril(jnp.ones((BLOCK, BLOCK), bool))

    def to_blocks(tensor):
        return tensor.reshape(blocks_count, BLOCK, heads_all, head_width)

    def advance(state_now, segment):
        query_seg, key_seg, decay_seg, value_seg = segment
        running = jnp.cumsum(decay_seg, axis=0)
        query_scaled = query_seg * jnp.exp(running)
        key_scaled = key_seg * jnp.exp(-running)
        scores = jnp.einsum('thd,shd->hts', query_scaled, key_scaled, precision=BEST_PRECISION)
        scores = jnp.where(tri_mask[None], scores, 0.0)
        result = jnp.einsum('hts,shv->thv', scores, value_seg, precision=BEST_PRECISION)
        result = result + jnp.einsum('thd,hdv->thv', query_scaled, state_now, precision=BEST_PRECISION)
        final_log = running[-1]
        state_next = jnp.exp(final_log)[:, :, None] * state_now + jnp.einsum('shd,shv->hdv', key_seg * jnp.exp(final_log[None] - running), value_seg, precision=BEST_PRECISION)
        return (state_next, result)
    initial = jnp.zeros((heads_all, head_width, head_width), jnp.float32)
    _, results = lax.scan(advance, initial, (to_blocks(query_f), to_blocks(key_f), to_blocks(decay_f), to_blocks(value_f)))
    return results.reshape(total_rows, heads_all, head_width)

def reference(queries, forget_logits, value_matrix, output_gate_logits, forget_slack, spike_log_forget, head_norm_gain, output_weight, residual, mixer_norm_gain, mixer_gate_weight, mixer_up_weight, mixer_down_weight):
    total_rows = queries.shape[0]
    query_f = (jax.nn.silu(queries.astype(jnp.float32)) * HEAD ** (-0.5)).reshape(total_rows, HEADS, HEAD)
    value_f = value_matrix.astype(jnp.float32).reshape(total_rows, HEADS, HEAD)
    gate_random_key = (forget_slack * jax.nn.sigmoid(-forget_logits.astype(jnp.float32))).reshape(2, total_rows, HEADS, HEAD)
    decay_logarithm = jnp.log1p(-gate_random_key) + spike_log_forget[None, :, :, None]
    forward_out = full_sweep(query_f, gate_random_key[0], decay_logarithm[0], value_f)
    backward_out = jnp.flip(full_sweep(jnp.flip(query_f, 0), jnp.flip(gate_random_key[1], 0), jnp.flip(decay_logarithm[1], 0), jnp.flip(value_f, 0)), 0)
    mixture = forward_out + backward_out
    mixed = (rms_scale(mixture, head_norm_gain).reshape(total_rows, HEADS * HEAD) * jax.nn.silu(output_gate_logits.astype(jnp.float32))).astype(jnp.bfloat16)
    group_cols = HEADS * HEAD // N_TP
    summed = residual.astype(jnp.float32)
    for group_index in range(N_TP):
        low_col = group_index * group_cols
        partial_out = jnp.dot(mixed[:, low_col:low_col + group_cols], output_weight[low_col:low_col + group_cols], preferred_element_type=jnp.float32).astype(jnp.bfloat16)
        summed = summed + lax.optimization_barrier(partial_out).astype(jnp.float32)
    hidden_state = summed.astype(jnp.bfloat16)
    unit_cols = FF // N_TP

    def channel_mix(hidden_seg):
        normed = rms_scale(hidden_seg.astype(jnp.float32), mixer_norm_gain).astype(jnp.bfloat16)
        gate_act = jnp.dot(normed, mixer_gate_weight, preferred_element_type=jnp.float32)
        up_act = jnp.dot(normed, mixer_up_weight, preferred_element_type=jnp.float32)
        inner = (jax.nn.silu(gate_act) * up_act).astype(jnp.bfloat16)
        summed_seg = hidden_seg.astype(jnp.float32)
        for group_index in range(N_TP):
            low_unit = group_index * unit_cols
            lowered = jnp.dot(inner[:, low_unit:low_unit + unit_cols], mixer_down_weight[low_unit:low_unit + unit_cols], preferred_element_type=jnp.float32).astype(jnp.bfloat16)
            summed_seg = summed_seg + lax.optimization_barrier(lowered).astype(jnp.float32)
        return summed_seg.astype(jnp.bfloat16)
    hidden_blocks = hidden_state.reshape(total_rows // TOK_DEV, TOK_DEV, D)
    return lax.map(channel_mix, hidden_blocks).reshape(total_rows, D)
```

```python
import functools

import jax
import jax.numpy as jnp
from jax import lax
from jax.experimental import pallas as pl
from jax.experimental.pallas import tpu as pltpu
from jax.sharding import PartitionSpec as P

NORM_EPS = 1e-06
MESH = pl.DeviceIdType.MESH
PAD_ROWS = 16
GROUP = 8


def dot_nt(a, b):
    return lax.dot_general(a, b, (((1,), (1,)), ((), ())), preferred_element_type=jnp.float32)


def dot_tn(a, b):
    return lax.dot_general(a, b, (((0,), (0,)), ((), ())), preferred_element_type=jnp.float32)


def dot_nn(a, b):
    return jnp.dot(a, b, preferred_element_type=jnp.float32)


def silu(x):
    return x * jax.nn.sigmoid(x)


def split_bf16(x):
    high = x.astype(jnp.bfloat16)
    return high, (x - high.astype(jnp.float32)).astype(jnp.bfloat16)


def sweep_kernel(q_ref, f_ref, v_ref, slack_ref, spike_ref, local_ref, reach_ref, state_ref):
    head = pl.program_id(0)
    rows, width = q_ref.shape
    query = silu(q_ref[...].astype(jnp.float32)) * (width ** -0.5)
    value = v_ref[...]
    spikes = spike_ref[...]
    lane = lax.broadcasted_iota(jnp.int32, spikes.shape, 1)
    spike = jnp.sum(jnp.where(lane == head, spikes, 0.0), axis=1, keepdims=True)
    slack = slack_ref[...]
    down = lax.broadcasted_iota(jnp.int32, (rows, rows), 0)
    across = lax.broadcasted_iota(jnp.int32, (rows, rows), 1)
    scores = None
    for way in (0, 1):
        mask = (down >= across) if way == 0 else (down <= across)
        tri = jnp.where(mask, 1.0, 0.0).astype(jnp.bfloat16)
        key = slack * jax.nn.sigmoid(-f_ref[way].astype(jnp.float32))
        decay = jnp.log1p(-key) + spike
        high, low = split_bf16(decay)
        running = dot_nn(tri, high) + dot_nn(tri, low)
        final = running[rows - 1 : rows] if way == 0 else running[0:1]
        query_scaled = (query * jnp.exp(running)).astype(jnp.bfloat16)
        key_scaled = (key * jnp.exp(-running)).astype(jnp.bfloat16)
        key_end = (key * jnp.exp(final - running)).astype(jnp.bfloat16)
        part = jnp.where(mask, dot_nt(query_scaled, key_scaled), 0.0)
        scores = part if scores is None else scores + part
        reach_ref[way] = query_scaled
        state_ref[way, 0, 0:width] = dot_tn(value, key_end).astype(jnp.bfloat16)
        total_high, total_low = split_bf16(jnp.exp(final))
        place = lax.broadcasted_iota(jnp.int32, (PAD_ROWS, width), 0)
        state_ref[way, 0, width : width + PAD_ROWS] = jnp.where(
            place == 0,
            total_high.astype(jnp.float32),
            jnp.where(place == 1, total_low.astype(jnp.float32), 0.0),
        ).astype(jnp.bfloat16)
    local_ref[...] = dot_nn(scores.astype(jnp.bfloat16), value)


def sweep(queries, forget_logits, values, slack, spike):
    rows, columns = queries.shape
    heads = spike.shape[1]
    width = columns // heads
    by_head = pl.BlockSpec((rows, width), lambda h: (0, h))
    return pl.pallas_call(
        sweep_kernel,
        grid=(heads,),
        in_specs=[
            by_head,
            pl.BlockSpec((2, rows, width), lambda h: (0, 0, h)),
            by_head,
            pl.BlockSpec((1, width), lambda h: (0, h)),
            pl.BlockSpec((rows, heads), lambda h: (0, 0)),
        ],
        out_specs=[
            by_head,
            pl.BlockSpec((2, rows, width), lambda h: (0, 0, h)),
            pl.BlockSpec((2, 1, width + PAD_ROWS, width), lambda h: (0, h, 0, 0)),
        ],
        out_shape=[
            jax.ShapeDtypeStruct((rows, columns), jnp.float32),
            jax.ShapeDtypeStruct((2, rows, columns), jnp.bfloat16),
            jax.ShapeDtypeStruct((2, heads, width + PAD_ROWS, width), jnp.bfloat16),
        ],
        cost_estimate=pl.CostEstimate(
            flops=20 * rows * width * columns, bytes_accessed=8 * rows * columns, transcendentals=8 * rows * columns
        ),
        name="sweep",
    )(queries, forget_logits, values, slack.reshape(1, columns), spike)


def greet(axis, others, count):
    barrier = pltpu.get_barrier_semaphore()

    def signal(k, carry):
        pl.semaphore_signal(barrier, inc=1, device_id={axis: others(k)}, device_id_type=MESH)
        return carry

    lax.fori_loop(1, count, signal, 0)
    pl.semaphore_wait(barrier, count - 1)


def exchange_kernel(n, state_ref, enter_ref, held, made, out_sem, in_sem, out_sem2, in_sem2):
    me = lax.axis_index("sp")
    rows = enter_ref.shape[1]

    def other(k):
        return lax.rem(me + k, n)

    greet("sp", other, n)

    def first(k):
        there = other(k)
        return pltpu.make_async_remote_copy(
            src_ref=state_ref.at[there],
            dst_ref=held.at[me],
            send_sem=out_sem.at[k],
            recv_sem=in_sem.at[k],
            device_id={"sp": there},
            device_id_type=MESH,
        )

    def second(k):
        there = other(k)
        return pltpu.make_async_remote_copy(
            src_ref=made.at[there],
            dst_ref=enter_ref.at[me],
            send_sem=out_sem2.at[k],
            recv_sem=in_sem2.at[k],
            device_id={"sp": there},
            device_id_type=MESH,
        )

    def go(copy):
        def start(k, carry):
            copy(k).start()
            return carry

        lax.fori_loop(1, n, start, 0)

    def end(copy):
        def wait(k, carry):
            copy(k).wait()
            return carry

        lax.fori_loop(1, n, wait, 0)

    go(first)
    held[me] = state_ref[me]
    end(first)
    backward = me // (n // 2)

    def step(i, total):
        source = i + backward * (n - 1 - 2 * i)
        made[source] = total.astype(jnp.bfloat16)
        block = held[source].astype(jnp.float32)
        factor = block[rows : rows + 1] + block[rows + 1 : rows + 2]
        return factor * total + block[:rows]

    lax.fori_loop(0, n, step, jnp.zeros(enter_ref.shape[1:], jnp.float32))
    go(second)
    enter_ref[me] = made[me]
    end(second)


def exchange(states):
    n = lax.axis_size("sp")
    ways, heads, padded, width = states.shape
    depth = padded - PAD_ROWS
    cuts = n // (ways * heads)
    rows = depth // cuts
    if cuts > 1:
        body = states[:, :, :depth].reshape(ways, heads, cuts, rows, width)
        tail = jnp.broadcast_to(
            states[:, :, None, depth:], (ways, heads, cuts, PAD_ROWS, width)
        )
        states = jnp.concatenate([body, tail], axis=3)
    entered = pl.pallas_call(
        functools.partial(exchange_kernel, n),
        in_specs=[pl.BlockSpec(memory_space=pltpu.VMEM)],
        out_specs=pl.BlockSpec(memory_space=pltpu.VMEM),
        out_shape=jax.ShapeDtypeStruct((n, rows, width), jnp.bfloat16),
        scratch_shapes=[
            pltpu.VMEM((n, rows + PAD_ROWS, width), jnp.bfloat16),
            pltpu.VMEM((n, rows, width), jnp.bfloat16),
            pltpu.SemaphoreType.DMA((n,)),
            pltpu.SemaphoreType.DMA((n,)),
            pltpu.SemaphoreType.DMA((n,)),
            pltpu.SemaphoreType.DMA((n,)),
        ],
        compiler_params=pltpu.CompilerParams(collective_id=1, has_side_effects=True),
        cost_estimate=pl.CostEstimate(flops=10**8, bytes_accessed=10**8, transcendentals=0),
        name="exchange",
    )(states.reshape(n, rows + PAD_ROWS, width))
    return entered.reshape(ways, heads, depth, width)


def reshard_kernel(g, *refs):
    count = (len(refs) - 3) // 2
    gives, takes = refs[:count], refs[count : 2 * count]
    out_sem, in_sem, own_sem = refs[2 * count :]
    me = lax.axis_index("sp")
    base = me // g * g
    seat = me - base

    def other(k):
        return lax.rem(seat + k, g)

    greet("sp", lambda k: base + other(k), g)
    copies = []
    for k in range(1, g):
        there = other(k)
        for i in range(count):
            copies.append(
                pltpu.make_async_remote_copy(
                    src_ref=gives[i].at[there],
                    dst_ref=takes[i].at[seat],
                    send_sem=out_sem.at[i, k],
                    recv_sem=in_sem.at[i, k],
                    device_id={"sp": base + there},
                    device_id_type=MESH,
                )
            )
            copies[-1].start()
    for i in range(count):
        copies.append(pltpu.make_async_copy(gives[i].at[seat], takes[i].at[seat], own_sem.at[i]))
        copies[-1].start()
    for copy in copies:
        copy.wait()


def reshard(arrays, g, collective_id):
    count = len(arrays)
    return pl.pallas_call(
        functools.partial(reshard_kernel, g),
        in_specs=[pl.BlockSpec(memory_space=pltpu.VMEM)] * count,
        out_specs=[pl.BlockSpec(memory_space=pltpu.VMEM)] * count,
        out_shape=[jax.ShapeDtypeStruct(a.shape, a.dtype) for a in arrays],
        scratch_shapes=[
            pltpu.SemaphoreType.DMA((count, g)),
            pltpu.SemaphoreType.DMA((count, g)),
            pltpu.SemaphoreType.DMA((count,)),
        ],
        compiler_params=pltpu.CompilerParams(
            collective_id=collective_id, has_side_effects=True
        ),
        cost_estimate=pl.CostEstimate(flops=10**8, bytes_accessed=10**8, transcendentals=0),
        name="reshard",
    )(*arrays)


def project_kernel(local_ref, reach_ref, enter_ref, gain_ref, gate_ref, weight_ref, out_ref, total):
    head = pl.program_id(0)
    mix = (
        local_ref[...]
        + dot_nt(reach_ref[0], enter_ref[0, 0])
        + dot_nt(reach_ref[1], enter_ref[1, 0])
    )
    scale = lax.rsqrt(jnp.mean(mix * mix, axis=-1, keepdims=True) + NORM_EPS)
    gate = silu(gate_ref[...].astype(jnp.float32))
    mixed = (mix * scale * gain_ref[...].astype(jnp.float32) * gate).astype(jnp.bfloat16)
    term = dot_nn(mixed, weight_ref[...])

    @pl.when(head == 0)
    def _():
        total[...] = term

    @pl.when(head > 0)
    def _():
        total[...] += term

    @pl.when(head == pl.num_programs(0) - 1)
    def _():
        out_ref[...] = total[...].astype(jnp.bfloat16)


def project(local, reach, entered, gain, gate_logits, weight):
    rows, columns = local.shape
    heads, width = entered.shape[1], entered.shape[3]
    model = weight.shape[1]
    by_head = pl.BlockSpec((rows, width), lambda h: (0, h))
    return pl.pallas_call(
        project_kernel,
        grid=(heads,),
        in_specs=[
            by_head,
            pl.BlockSpec((2, rows, width), lambda h: (0, 0, h)),
            pl.BlockSpec((2, 1, width, width), lambda h: (0, h, 0, 0)),
            pl.BlockSpec((1, width), lambda h: (0, 0)),
            by_head,
            pl.BlockSpec((width, model), lambda h: (h, 0)),
        ],
        out_specs=pl.BlockSpec((rows, model), lambda h: (0, 0)),
        out_shape=jax.ShapeDtypeStruct((rows, model), jnp.bfloat16),
        scratch_shapes=[pltpu.VMEM((rows, model), jnp.float32)],
        cost_estimate=pl.CostEstimate(
            flops=2 * rows * columns * model, bytes_accessed=2 * columns * model, transcendentals=rows * columns
        ),
        name="project",
    )(local, reach, entered, gain.reshape(1, width), gate_logits, weight)


def local(
    queries,
    forget_logits,
    value_matrix,
    output_gate_logits,
    forget_slack,
    spike_log_forget,
    head_norm_gain,
    output_weight,
    residual,
    mixer_norm_gain,
    mixer_gate_weight,
    mixer_up_weight,
    mixer_down_weight,
):
    n, tp = lax.axis_size("sp"), lax.axis_size("tp")
    g = GROUP
    row_count = queries.shape[0]
    depth, units = mixer_gate_weight.shape
    near = [[b * g + j for j in range(g)] for b in range(n // g)]
    far = [[b * g + j for b in range(n // g)] for j in range(g)]

    def cut(weight):
        return weight.reshape(depth, g, units // g).transpose(1, 0, 2)

    pieces = reshard([cut(mixer_gate_weight), cut(mixer_up_weight), cut(mixer_down_weight.T)], g, 2)
    gate_weight, up_weight, down_weight = (
        lax.all_gather(
            p.reshape(g * depth, units // g), "sp", axis=0, tiled=True, axis_index_groups=far
        )
        for p in pieces
    )

    local_out, reach, states = sweep(
        queries, forget_logits, value_matrix, forget_slack, spike_log_forget
    )
    entered = exchange(states)
    part = project(local_out, reach, entered, head_norm_gain, output_gate_logits, output_weight)
    part_rows = row_count // tp
    if tp > 1:
        part = lax.psum_scatter(part, "tp", scatter_dimension=0, tiled=True)
        residual = lax.dynamic_slice_in_dim(
            residual, lax.axis_index("tp") * part_rows, part_rows, 0
        )
    hidden = (residual.astype(jnp.float32) + part.astype(jnp.float32)).astype(jnp.bfloat16)
    hidden_f = hidden.astype(jnp.float32)
    normed = (
        hidden_f
        * lax.rsqrt(jnp.mean(hidden_f * hidden_f, axis=-1, keepdims=True) + NORM_EPS)
        * mixer_norm_gain.astype(jnp.float32)
    ).astype(jnp.bfloat16)
    normed = lax.all_gather(normed, "sp", axis=0, tiled=True, axis_index_groups=near)
    if tp > 1:
        normed = lax.all_gather(normed, "tp", axis=0, tiled=True)
    gate_act = dot_nn(normed, gate_weight)
    up_act = dot_nn(normed, up_weight)
    inner = (silu(gate_act) * up_act).astype(jnp.bfloat16)
    lowered = dot_nt(inner, down_weight).astype(jnp.bfloat16)
    if tp > 1:
        lowered = lax.psum_scatter(lowered, "tp", scatter_dimension=0, tiled=True)
    (terms,) = reshard([lowered.reshape(g, part_rows, lowered.shape[1])], g, 3)
    added = jnp.sum(terms.astype(jnp.float32), axis=0)
    return (hidden_f + added).astype(jnp.bfloat16)


def solution(mesh):
    placed = (
        P("sp", "tp"),
        P(None, "sp", "tp"),
        P("sp", "tp"),
        P("sp", "tp"),
        P("tp"),
        P("sp", "tp"),
        P(),
        P("tp", None),
        P("sp", None),
        P(),
        P("sp", "tp"),
        P("sp", "tp"),
        P("tp", "sp"),
    )
    return jax.shard_map(
        local, mesh=mesh, in_specs=placed, out_specs=P(("sp", "tp"), None), check_vma=False
    )
```

```python
import functools

import jax
import jax.numpy as jnp
from jax import lax
from jax.experimental import pallas as pl
from jax.experimental.pallas import tpu as pltpu
from jax.sharding import PartitionSpec as P

NORM_EPS = 1e-06
MESH = pl.DeviceIdType.MESH
PAD_ROWS = 16
GROUP = 8


def dot_nt(a, b):
    return lax.dot_general(a, b, (((1,), (1,)), ((), ())), preferred_element_type=jnp.float32)


def dot_tn(a, b):
    return lax.dot_general(a, b, (((0,), (0,)), ((), ())), preferred_element_type=jnp.float32)


def dot_nn(a, b):
    return jnp.dot(a, b, preferred_element_type=jnp.float32)


def silu(x):
    return x * jax.nn.sigmoid(x)


def split_bf16(x):
    high = x.astype(jnp.bfloat16)
    return high, (x - high.astype(jnp.float32)).astype(jnp.bfloat16)


def sweep_kernel(q_ref, f_ref, v_ref, slack_ref, spike_ref, local_ref, reach_ref, state_ref):
    head = pl.program_id(0)
    rows, width = q_ref.shape
    query = silu(q_ref[...].astype(jnp.float32)) * (width ** -0.5)
    value = v_ref[...]
    spikes = spike_ref[...]
    lane = lax.broadcasted_iota(jnp.int32, spikes.shape, 1)
    spike = jnp.sum(jnp.where(lane == head, spikes, 0.0), axis=1, keepdims=True)
    slack = slack_ref[...]
    down = lax.broadcasted_iota(jnp.int32, (rows, rows), 0)
    across = lax.broadcasted_iota(jnp.int32, (rows, rows), 1)
    scores = None
    for way in (0, 1):
        mask = (down >= across) if way == 0 else (down <= across)
        tri = jnp.where(mask, 1.0, 0.0).astype(jnp.bfloat16)
        key = slack * jax.nn.sigmoid(-f_ref[way].astype(jnp.float32))
        decay = jnp.log1p(-key) + spike
        high, low = split_bf16(decay)
        running = dot_nn(tri, high) + dot_nn(tri, low)
        final = running[rows - 1 : rows] if way == 0 else running[0:1]
        query_scaled = (query * jnp.exp(running)).astype(jnp.bfloat16)
        key_scaled = (key * jnp.exp(-running)).astype(jnp.bfloat16)
        key_end = (key * jnp.exp(final - running)).astype(jnp.bfloat16)
        part = jnp.where(mask, dot_nt(query_scaled, key_scaled), 0.0)
        scores = part if scores is None else scores + part
        reach_ref[way] = query_scaled
        state_ref[way, 0, 0:width] = dot_tn(value, key_end).astype(jnp.bfloat16)
        total_high, total_low = split_bf16(jnp.exp(final))
        place = lax.broadcasted_iota(jnp.int32, (PAD_ROWS, width), 0)
        state_ref[way, 0, width : width + PAD_ROWS] = jnp.where(
            place == 0,
            total_high.astype(jnp.float32),
            jnp.where(place == 1, total_low.astype(jnp.float32), 0.0),
        ).astype(jnp.bfloat16)
    local_ref[...] = dot_nn(scores.astype(jnp.bfloat16), value)


def sweep(queries, forget_logits, values, slack, spike):
    rows, columns = queries.shape
    heads = spike.shape[1]
    width = columns // heads
    by_head = pl.BlockSpec((rows, width), lambda h: (0, h))
    return pl.pallas_call(
        sweep_kernel,
        grid=(heads,),
        in_specs=[
            by_head,
            pl.BlockSpec((2, rows, width), lambda h: (0, 0, h)),
            by_head,
            pl.BlockSpec((1, width), lambda h: (0, h)),
            pl.BlockSpec((rows, heads), lambda h: (0, 0)),
        ],
        out_specs=[
            by_head,
            pl.BlockSpec((2, rows, width), lambda h: (0, 0, h)),
            pl.BlockSpec((2, 1, width + PAD_ROWS, width), lambda h: (0, h, 0, 0)),
        ],
        out_shape=[
            jax.ShapeDtypeStruct((rows, columns), jnp.float32),
            jax.ShapeDtypeStruct((2, rows, columns), jnp.bfloat16),
            jax.ShapeDtypeStruct((2, heads, width + PAD_ROWS, width), jnp.bfloat16),
        ],
        cost_estimate=pl.CostEstimate(
            flops=20 * rows * width * columns, bytes_accessed=8 * rows * columns, transcendentals=8 * rows * columns
        ),
        name="sweep",
    )(queries, forget_logits, values, slack.reshape(1, columns), spike)


def greet(axis, others, count):
    barrier = pltpu.get_barrier_semaphore()

    def signal(k, carry):
        pl.semaphore_signal(barrier, inc=1, device_id={axis: others(k)}, device_id_type=MESH)
        return carry

    lax.fori_loop(1, count, signal, 0)
    pl.semaphore_wait(barrier, count - 1)


def exchange_kernel(n, state_ref, enter_ref, held, made, out_sem, in_sem, out_sem2, in_sem2):
    me = lax.axis_index("sp")
    rows = enter_ref.shape[1]

    def other(k):
        return lax.rem(me + k, n)

    greet("sp", other, n)

    def first(k):
        there = other(k)
        return pltpu.make_async_remote_copy(
            src_ref=state_ref.at[there],
            dst_ref=held.at[me],
            send_sem=out_sem.at[k],
            recv_sem=in_sem.at[k],
            device_id={"sp": there},
            device_id_type=MESH,
        )

    def second(k):
        there = other(k)
        return pltpu.make_async_remote_copy(
            src_ref=made.at[there],
            dst_ref=enter_ref.at[me],
            send_sem=out_sem2.at[k],
            recv_sem=in_sem2.at[k],
            device_id={"sp": there},
            device_id_type=MESH,
        )

    def go(copy):
        def start(k, carry):
            copy(k).start()
            return carry

        lax.fori_loop(1, n, start, 0)

    def end(copy):
        def wait(k, carry):
            copy(k).wait()
            return carry

        lax.fori_loop(1, n, wait, 0)

    go(first)
    held[me] = state_ref[me]
    end(first)
    backward = me // (n // 2)

    def step(i, total):
        source = i + backward * (n - 1 - 2 * i)
        made[source] = total.astype(jnp.bfloat16)
        block = held[source].astype(jnp.float32)
        factor = block[rows : rows + 1] + block[rows + 1 : rows + 2]
        return factor * total + block[:rows]

    lax.fori_loop(0, n, step, jnp.zeros(enter_ref.shape[1:], jnp.float32))
    go(second)
    enter_ref[me] = made[me]
    end(second)


def exchange(states):
    n = lax.axis_size("sp")
    ways, heads, padded, width = states.shape
    depth = padded - PAD_ROWS
    cuts = n // (ways * heads)
    rows = depth // cuts
    if cuts > 1:
        body = states[:, :, :depth].reshape(ways, heads, cuts, rows, width)
        tail = jnp.broadcast_to(
            states[:, :, None, depth:], (ways, heads, cuts, PAD_ROWS, width)
        )
        states = jnp.concatenate([body, tail], axis=3)
    entered = pl.pallas_call(
        functools.partial(exchange_kernel, n),
        in_specs=[pl.BlockSpec(memory_space=pltpu.VMEM)],
        out_specs=pl.BlockSpec(memory_space=pltpu.VMEM),
        out_shape=jax.ShapeDtypeStruct((n, rows, width), jnp.bfloat16),
        scratch_shapes=[
            pltpu.VMEM((n, rows + PAD_ROWS, width), jnp.bfloat16),
            pltpu.VMEM((n, rows, width), jnp.bfloat16),
            pltpu.SemaphoreType.DMA((n,)),
            pltpu.SemaphoreType.DMA((n,)),
            pltpu.SemaphoreType.DMA((n,)),
            pltpu.SemaphoreType.DMA((n,)),
        ],
        compiler_params=pltpu.CompilerParams(collective_id=1, has_side_effects=True),
        name="exchange",
    )(states.reshape(n, rows + PAD_ROWS, width))
    return entered.reshape(ways, heads, depth, width)


def reshard_kernel(g, *refs):
    count = (len(refs) - 3) // 2
    gives, takes = refs[:count], refs[count : 2 * count]
    out_sem, in_sem, own_sem = refs[2 * count :]
    me = lax.axis_index("sp")
    base = me // g * g
    seat = me - base

    def other(k):
        return lax.rem(seat + k, g)

    greet("sp", lambda k: base + other(k), g)
    copies = []
    for k in range(1, g):
        there = other(k)
        for i in range(count):
            copies.append(
                pltpu.make_async_remote_copy(
                    src_ref=gives[i].at[there],
                    dst_ref=takes[i].at[seat],
                    send_sem=out_sem.at[i, k],
                    recv_sem=in_sem.at[i, k],
                    device_id={"sp": base + there},
                    device_id_type=MESH,
                )
            )
            copies[-1].start()
    for i in range(count):
        copies.append(pltpu.make_async_copy(gives[i].at[seat], takes[i].at[seat], own_sem.at[i]))
        copies[-1].start()
    for copy in copies:
        copy.wait()


def reshard(arrays, g, collective_id):
    count = len(arrays)
    return pl.pallas_call(
        functools.partial(reshard_kernel, g),
        in_specs=[pl.BlockSpec(memory_space=pltpu.VMEM)] * count,
        out_specs=[pl.BlockSpec(memory_space=pltpu.VMEM)] * count,
        out_shape=[jax.ShapeDtypeStruct(a.shape, a.dtype) for a in arrays],
        scratch_shapes=[
            pltpu.SemaphoreType.DMA((count, g)),
            pltpu.SemaphoreType.DMA((count, g)),
            pltpu.SemaphoreType.DMA((count,)),
        ],
        compiler_params=pltpu.CompilerParams(
            collective_id=collective_id, has_side_effects=True
        ),
        name="reshard",
    )(*arrays)


def gather_kernel(g, give, take, out_sem, in_sem):
    me = lax.axis_index("sp")
    base = me // g * g
    seat = me - base

    def other(k):
        return lax.rem(seat + k, g)

    greet("sp", lambda k: base + other(k), g)
    copies = []
    for k in range(1, g):
        copies.append(
            pltpu.make_async_remote_copy(
                src_ref=give,
                dst_ref=take.at[seat],
                send_sem=out_sem.at[k],
                recv_sem=in_sem.at[k],
                device_id={"sp": base + other(k)},
                device_id_type=MESH,
            )
        )
        copies[-1].start()
    take[seat] = give[...]
    for copy in copies:
        copy.wait()


def gather(array, g, collective_id):
    return pl.pallas_call(
        functools.partial(gather_kernel, g),
        in_specs=[pl.BlockSpec(memory_space=pltpu.VMEM)],
        out_specs=pl.BlockSpec(memory_space=pltpu.VMEM),
        out_shape=jax.ShapeDtypeStruct((g,) + array.shape, array.dtype),
        scratch_shapes=[pltpu.SemaphoreType.DMA((g,)), pltpu.SemaphoreType.DMA((g,))],
        compiler_params=pltpu.CompilerParams(
            collective_id=collective_id, has_side_effects=True
        ),
        name="gather",
    )(array).reshape((g * array.shape[0],) + array.shape[1:])


def project_kernel(local_ref, reach_ref, enter_ref, gain_ref, gate_ref, weight_ref, out_ref, total):
    head = pl.program_id(0)
    mix = (
        local_ref[...]
        + dot_nt(reach_ref[0], enter_ref[0, 0])
        + dot_nt(reach_ref[1], enter_ref[1, 0])
    )
    scale = lax.rsqrt(jnp.mean(mix * mix, axis=-1, keepdims=True) + NORM_EPS)
    gate = silu(gate_ref[...].astype(jnp.float32))
    mixed = (mix * scale * gain_ref[...].astype(jnp.float32) * gate).astype(jnp.bfloat16)
    term = dot_nn(mixed, weight_ref[...])

    @pl.when(head == 0)
    def _():
        total[...] = term

    @pl.when(head > 0)
    def _():
        total[...] += term

    @pl.when(head == pl.num_programs(0) - 1)
    def _():
        out_ref[...] = total[...].astype(jnp.bfloat16)


def project(local, reach, entered, gain, gate_logits, weight):
    rows, columns = local.shape
    heads, width = entered.shape[1], entered.shape[3]
    model = weight.shape[1]
    by_head = pl.BlockSpec((rows, width), lambda h: (0, h))
    return pl.pallas_call(
        project_kernel,
        grid=(heads,),
        in_specs=[
            by_head,
            pl.BlockSpec((2, rows, width), lambda h: (0, 0, h)),
            pl.BlockSpec((2, 1, width, width), lambda h: (0, h, 0, 0)),
            pl.BlockSpec((1, width), lambda h: (0, 0)),
            by_head,
            pl.BlockSpec((width, model), lambda h: (h, 0)),
        ],
        out_specs=pl.BlockSpec((rows, model), lambda h: (0, 0)),
        out_shape=jax.ShapeDtypeStruct((rows, model), jnp.bfloat16),
        scratch_shapes=[pltpu.VMEM((rows, model), jnp.float32)],
        cost_estimate=pl.CostEstimate(
            flops=2 * rows * columns * model, bytes_accessed=2 * columns * model, transcendentals=rows * columns
        ),
        name="project",
    )(local, reach, entered, gain.reshape(1, width), gate_logits, weight)


def local(
    queries,
    forget_logits,
    value_matrix,
    output_gate_logits,
    forget_slack,
    spike_log_forget,
    head_norm_gain,
    output_weight,
    residual,
    mixer_norm_gain,
    mixer_gate_weight,
    mixer_up_weight,
    mixer_down_weight,
):
    n, tp = lax.axis_size("sp"), lax.axis_size("tp")
    g = GROUP
    row_count = queries.shape[0]
    depth, units = mixer_gate_weight.shape
    far = [[b * g + j for b in range(n // g)] for j in range(g)]

    def cut(weight):
        return weight.reshape(depth, g, units // g).transpose(1, 0, 2)

    pieces = reshard([cut(mixer_gate_weight), cut(mixer_up_weight), cut(mixer_down_weight.T)], g, 2)
    gate_weight, up_weight, down_weight = (
        lax.all_gather(
            p.reshape(g * depth, units // g), "sp", axis=0, tiled=True, axis_index_groups=far
        )
        for p in pieces
    )

    local_out, reach, states = sweep(
        queries, forget_logits, value_matrix, forget_slack, spike_log_forget
    )
    entered = exchange(states)
    part = project(local_out, reach, entered, head_norm_gain, output_gate_logits, output_weight)
    part_rows = row_count // tp
    if tp > 1:
        part = lax.psum_scatter(part, "tp", scatter_dimension=0, tiled=True)
        residual = lax.dynamic_slice_in_dim(
            residual, lax.axis_index("tp") * part_rows, part_rows, 0
        )
    hidden = (residual.astype(jnp.float32) + part.astype(jnp.float32)).astype(jnp.bfloat16)
    hidden_f = hidden.astype(jnp.float32)
    normed = (
        hidden_f
        * lax.rsqrt(jnp.mean(hidden_f * hidden_f, axis=-1, keepdims=True) + NORM_EPS)
        * mixer_norm_gain.astype(jnp.float32)
    ).astype(jnp.bfloat16)
    normed = gather(normed, g, 4)
    if tp > 1:
        normed = lax.all_gather(normed, "tp", axis=0, tiled=True)
    gate_act = dot_nn(normed, gate_weight)
    up_act = dot_nn(normed, up_weight)
    inner = (silu(gate_act) * up_act).astype(jnp.bfloat16)
    lowered = dot_nt(inner, down_weight).astype(jnp.bfloat16)
    if tp > 1:
        lowered = lax.psum_scatter(lowered, "tp", scatter_dimension=0, tiled=True)
    (terms,) = reshard([lowered.reshape(g, part_rows, lowered.shape[1])], g, 3)
    added = jnp.sum(terms.astype(jnp.float32), axis=0)
    return (hidden_f + added).astype(jnp.bfloat16)


def solution(mesh):
    placed = (
        P("sp", "tp"),
        P(None, "sp", "tp"),
        P("sp", "tp"),
        P("sp", "tp"),
        P("tp"),
        P("sp", "tp"),
        P(),
        P("tp", None),
        P("sp", None),
        P(),
        P("sp", "tp"),
        P("sp", "tp"),
        P("tp", "sp"),
    )
    return jax.shard_map(
        local, mesh=mesh, in_specs=placed, out_specs=P(("sp", "tp"), None), check_vma=False
    )
```
